32 devices in a mesh: grp: 2 (over y), sp: 4 (over z), tp: 4 (over x, core).
Axes of the slice: x: 2, y: 2, z: 4, core: 2. Of those that a mesh axis runs over, the one named last changes fastest.
Arguments:
- latent: bfloat16 [2048, 2048], P(('grp', 'sp', 'tp')), parts along dimension 0, may hold values from -6 to 6
- cond: bfloat16 [4096], P(('grp', 'sp')), parts along dimension 0, may hold values from -6 to 6
- context: bfloat16 [512, 2048], P(('grp', 'sp')), parts along dimension 0, may hold values from -6 to 6
- context_cond: bfloat16 [2048], P('sp'), may hold values from -6 to 6
- norm_gain: bfloat16 [2048], replicated, may hold values from 0.099609375 to 1.8984375
- mod_shift: bfloat16 [2048, 2048], P('sp', 'tp'), may hold values from -0.125 to 0.125
- mod_scale: bfloat16 [2048, 2048], P('sp', 'tp'), may hold values from -0.125 to 0.125
- mod_gate: bfloat16 [2048, 2048], P('sp', 'tp'), may hold values from -0.125 to 0.125
- w_query: bfloat16 [2048, 2048], P(None, 'tp'), may hold values from -0.125 to 0.125
- w_key: bfloat16 [2048, 2048], P(None, 'tp'), may hold values from -0.125 to 0.125
- w_value: bfloat16 [2048, 4096], P(None, 'tp'), may hold values from -0.125 to 0.125
- w_gate: bfloat16 [2048, 4096], P(None, 'tp'), may hold values from -0.125 to 0.125
- w_out: bfloat16 [4096, 2048], P('tp'), may hold values from -0.09375 to 0.09375
- decay_rate: float32 [2, 8], P(None, 'tp'), may hold values from 0.00015625 to 0.034
- context_gain: float32 [8], P('tp'), may hold values from 3 to 10
Outputs:
- mixed: bfloat16 [2048, 2048], P(('grp', 'sp', 'tp')), parts along dimension 0
The draws below stay inside these ranges and needn't reach their ends.
There are 2 independent parts, one for each index of `grp`. The reference program is written for one: setup_inputs(seed, part) draws one part's arguments, and reference() takes and returns one part's arrays. A program takes and returns all parts, laid end to end along the dimension named above; an argument that names none is the same for every part. Nothing has to cross between parts.
All inputs are finite; a program needn't handle non-finite values.
Results may differ from the reference program's by a relative error of at most 0.009.
Values may be sent and summed in bfloat16 or wider, within the bound.
A program may use at most 128 MiB of HBM per device.

```python
import math
import jax
import jax.numpy as jnp
from jax import lax

D = 2048
H = 8
DK = 256
DV = 512
GRID_W = 128
BLOCK = 128
NL = 1024
CTX = 256
N_TP = 4


def draw_decay_rate(key, part):
    base = jax.random.fold_in(key, 17)
    pick_key, fast_key, slow_key = jax.random.split(base, 3)
    share = 0.5
    fast = jax.random.uniform(pick_key, (2, H), jnp.float32) < share
    fast_rate = jnp.exp(jax.random.uniform(fast_key, (2, H), jnp.float32, math.log(1.0 / 100.0), math.log(1.0 / 30.0)))
    slow_rate = jnp.exp(jax.random.uniform(slow_key, (2, H), jnp.float32, math.log(0.2), math.log(2.0))) / (NL + CTX)
    return jnp.where(fast, fast_rate, slow_rate).astype(jnp.float32)


def level_of(rng, extent, cuts, low, high):
    factor_of = 1.0
    for position, shards_of in cuts:
        heights = jax.random.uniform(jax.random.fold_in(jax.random.fold_in(rng, 6), position), (shards_of,), jnp.float32, low / len(cuts), high / len(cuts))
        factor_of = factor_of * jnp.repeat(jnp.exp(heights), extent[position] // shards_of).reshape((-1,) + (1,) * (len(extent) - 1 - position))
    return factor_of


def gaussian(key, shape, scale, reach, cuts=(), kind=jnp.bfloat16):
    entries = scale * jax.random.normal(key, shape, jnp.float32)
    if cuts:
        entries = entries * level_of(key, shape, cuts, -0.22, 0.18)
    return jnp.clip(entries, -reach, reach).astype(kind)


def setup_inputs(seed: int = 0, part: int = 0) -> dict:
    arg_keys = jax.random.split(jax.random.key(seed), 16)
    own_keys = jax.random.split(jax.random.fold_in(arg_keys[15], part), 16)
    latent = gaussian(own_keys[0], (NL, D), 1.0, 6.0, ((0, 16),))
    cond = gaussian(own_keys[1], (D,), 1.0, 6.0, ((0, 4),))
    context = gaussian(own_keys[2], (CTX, D), 1.0, 6.0, ((0, 4),))
    context_cond = gaussian(arg_keys[3], (D,), 1.0, 6.0, ((0, 4),))
    norm_gain = jnp.clip(1.0 + 0.18 * jax.random.normal(arg_keys[4], (D,), jnp.float32), 0.099609375, 1.8984375).astype(jnp.bfloat16)
    mod_shift = gaussian(arg_keys[5], (D, D), D ** -0.5, 0.125, ((0, 4), (1, 4)))
    mod_scale = gaussian(arg_keys[6], (D, D), D ** -0.5, 0.125, ((0, 4), (1, 4)))
    mod_gate = gaussian(arg_keys[7], (D, D), D ** -0.5, 0.125, ((0, 4), (1, 4)))
    w_query = gaussian(arg_keys[8], (D, H * DK), D ** -0.5, 0.125, ((1, 4),))
    w_key = gaussian(arg_keys[9], (D, H * DK), D ** -0.5, 0.125, ((1, 4),))
    w_value = gaussian(arg_keys[10], (D, H * DV), D ** -0.5, 0.125, ((1, 4),))
    w_gate = gaussian(arg_keys[11], (D, H * DV), D ** -0.5, 0.125, ((1, 4),))
    w_out = gaussian(arg_keys[12], (H * DV, D), (H * DV) ** -0.5, 0.09375, ((0, 4),))
    decay_rate = draw_decay_rate(jax.random.fold_in(arg_keys[15], 71), part)
    context_gain = jnp.clip(jnp.exp(math.log(10.0) - 1.2039728 * jax.random.uniform(arg_keys[14], (H,), jnp.float32) ** level_of(arg_keys[14], (H,), ((0, 4),), -0.2, 0.2)), 3.0, 10.0)
    return {"latent": latent, "cond": cond, "context": context, "context_cond": context_cond, "norm_gain": norm_gain, "mod_shift": mod_shift, "mod_scale": mod_scale, "mod_gate": mod_gate, "w_query": w_query, "w_key": w_key, "w_value": w_value, "w_gate": w_gate, "w_out": w_out, "decay_rate": decay_rate, "context_gain": context_gain}


norm_eps = 1e-06
rope_base = 10000.0
highest = lax.Precision.HIGHEST

def modulated(rows, norm_gain, shift, scale):
    values = rows.astype(jnp.float32)
    normed = values * lax.rsqrt(lax.optimization_barrier(jnp.mean(values * values, axis=-1, keepdims=True)) + norm_eps)
    return (normed * norm_gain.astype(jnp.float32) * (1.0 + scale) + shift).astype(jnp.bfloat16)

def rotate(vectors, positions):
    depth = vectors.shape[-1]
    freqs = depth // 4
    inv_freq = rope_base ** (-jnp.arange(freqs, dtype=jnp.float32) / freqs)
    grid_row = (positions // GRID_W).astype(jnp.float32)
    grid_col = (positions % GRID_W).astype(jnp.float32)
    angles = jnp.concatenate([grid_row[:, None] * inv_freq, grid_col[:, None] * inv_freq], axis=-1)[:, None, :]
    cos_table = jnp.cos(angles)
    sin_table = jnp.sin(angles)
    first_half, second_half = jnp.split(vectors, 2, axis=-1)
    return jnp.concatenate([first_half * cos_table - second_half * sin_table, second_half * cos_table + first_half * sin_table], axis=-1)

def rounded(values):
    return lax.optimization_barrier(values.astype(jnp.bfloat16)).astype(jnp.float32)

def context_states(ctx_key, ctx_value, fwd_rate, bwd_rate, context_gain):
    total = ctx_key.shape[0]
    place = jnp.arange(total, dtype=jnp.float32)[:, None]
    fwd_weight = jnp.exp(-fwd_rate[None, :] * (total - 1.0 - place))
    bwd_weight = jnp.exp(-bwd_rate[None, :] * place)
    keys_f = lax.optimization_barrier(ctx_key).astype(jnp.float32)
    values_f = lax.optimization_barrier(ctx_value).astype(jnp.float32)
    fwd_keys = rounded(keys_f * fwd_weight[:, :, None])
    bwd_keys = rounded(keys_f * bwd_weight[:, :, None])
    fwd_state = jnp.einsum('jhd,jhe->hde', fwd_keys, values_f, precision=highest)
    bwd_state = jnp.einsum('jhd,jhe->hde', bwd_keys, values_f, precision=highest)
    return (fwd_state * context_gain[:, None, None], bwd_state * context_gain[:, None, None])

def reference(latent, cond, context, context_cond, norm_gain, mod_shift, mod_scale, mod_gate, w_query, w_key, w_value, w_gate, w_out, decay_rate, context_gain):
    cond_rows = jax.nn.silu(jnp.stack([cond, context_cond]).astype(jnp.float32)).astype(jnp.bfloat16)
    shift = jnp.dot(cond_rows, mod_shift, preferred_element_type=jnp.float32)
    scale = jnp.dot(cond_rows, mod_scale, preferred_element_type=jnp.float32)
    gate = jnp.dot(cond_rows[0:1], mod_gate, preferred_element_type=jnp.float32)
    h_latent = modulated(latent, norm_gain, shift[0], scale[0])
    h_context = modulated(context, norm_gain, shift[1], scale[1])
    positions = jnp.arange(NL, dtype=jnp.int32)
    query = rotate(jnp.dot(h_latent, w_query, preferred_element_type=jnp.float32).reshape(NL, H, DK), positions).astype(jnp.bfloat16)
    keys = rotate(jnp.dot(h_latent, w_key, preferred_element_type=jnp.float32).reshape(NL, H, DK) * DK ** (-0.5), positions).astype(jnp.bfloat16)
    values = jnp.dot(h_latent, w_value, preferred_element_type=jnp.float32).astype(jnp.bfloat16).reshape(NL, H, DV)
    gate_pre = jnp.dot(h_latent, w_gate, preferred_element_type=jnp.float32).reshape(NL, H, DV)
    ctx_key = (jnp.dot(h_context, w_key, preferred_element_type=jnp.float32) * DK ** (-0.5)).astype(jnp.bfloat16)
    ctx_value = jnp.dot(h_context, w_value, preferred_element_type=jnp.float32).astype(jnp.bfloat16)
    fwd_rate = decay_rate[0]
    bwd_rate = decay_rate[1]
    ctx_fwd, ctx_bwd = context_states(ctx_key.reshape(CTX, H, DK), ctx_value.reshape(CTX, H, DV), fwd_rate, bwd_rate, context_gain)
    blocks = NL // BLOCK
    query_f = lax.optimization_barrier(query).astype(jnp.float32).reshape(blocks, BLOCK, H, DK)
    keys_f = lax.optimization_barrier(keys).astype(jnp.float32).reshape(blocks, BLOCK, H, DK)
    values_f = lax.optimization_barrier(values).astype(jnp.float32).reshape(blocks, BLOCK, H, DV)
    place = jnp.arange(BLOCK, dtype=jnp.float32)
    gap = place[:, None] - place[None, :]
    mask = jnp.where(gap >= 0, jnp.exp(-fwd_rate[:, None, None] * jnp.maximum(gap, 0.0)), 0.0) + jnp.where(gap <= 0, jnp.exp(-bwd_rate[:, None, None] * jnp.maximum(-gap, 0.0)), 0.0)
    scores = jnp.einsum('bihd,bjhd->bhij', query_f, keys_f, precision=highest)
    weights = lax.optimization_barrier((scores * mask[None]).astype(jnp.bfloat16)).astype(jnp.float32)
    retained = jnp.einsum('bhij,bjhe->bihe', weights, values_f, precision=highest)
    fwd_qw = jnp.exp(-fwd_rate[None, :] * (place[:, None] + 1.0))
    bwd_qw = jnp.exp(-bwd_rate[None, :] * (BLOCK - place[:, None]))
    fwd_kw = jnp.exp(-fwd_rate[None, :] * (BLOCK - 1.0 - place[:, None]))
    bwd_kw = jnp.exp(-bwd_rate[None, :] * place[:, None])
    fwd_keys = rounded(keys_f * fwd_kw[None, :, :, None])
    bwd_keys = rounded(keys_f * bwd_kw[None, :, :, None])
    fwd_step_decay = jnp.exp(-fwd_rate * BLOCK)[:, None, None]
    bwd_step_decay = jnp.exp(-bwd_rate * BLOCK)[:, None, None]

    def fwd_step(state, block):
        block_query, block_keys, block_values = block
        cross = jnp.einsum('ihd,hde->ihe', block_query, rounded(state), precision=highest) * fwd_qw[:, :, None]
        added = jnp.einsum('jhd,jhe->hde', block_keys, block_values, precision=highest)
        return (fwd_step_decay * state + added, cross)

    def bwd_step(state, block):
        block_query, block_keys, block_values = block
        cross = jnp.einsum('ihd,hde->ihe', block_query, rounded(state), precision=highest) * bwd_qw[:, :, None]
        added = jnp.einsum('jhd,jhe->hde', block_keys, block_values, precision=highest)
        return (bwd_step_decay * state + added, cross)
    fwd_final, fwd_cross = lax.scan(fwd_step, ctx_fwd, (query_f, fwd_keys, values_f))
    bwd_final, bwd_cross = lax.scan(bwd_step, ctx_bwd, (query_f, bwd_keys, values_f), reverse=True)
    retained = (retained + fwd_cross + bwd_cross).reshape(NL, H, DV)
    centre = lax.optimization_barrier(jnp.mean(retained, axis=-1, keepdims=True))
    variance = lax.optimization_barrier(jnp.mean(jnp.square(retained - centre), axis=-1, keepdims=True))
    normed = (retained - centre) * lax.rsqrt(variance + norm_eps)
    gated = (jax.nn.silu(gate_pre) * normed).astype(jnp.bfloat16).reshape(NL, H * DV)
    group_cols = H // N_TP * DV
    total = jnp.zeros((NL, D), jnp.float32)
    for group in range(N_TP):
        lower = group * group_cols
        partial_sum = jnp.dot(gated[:, lower:lower + group_cols], w_out[lower:lower + group_cols], preferred_element_type=jnp.float32).astype(jnp.bfloat16)
        total = total + lax.optimization_barrier(partial_sum).astype(jnp.float32)
    return (latent.astype(jnp.float32) + gate[0] * total).astype(jnp.bfloat16)
```

```python
import functools
import math

import jax
import jax.numpy as jnp
from jax import lax
from jax.experimental import pallas as pl
from jax.experimental.pallas import tpu as pltpu
from jax.sharding import PartitionSpec as P

DK = 256
GRID_W = 128
TILE = 256
CHUNK = 64
LAG = 2
norm_eps = 1e-06
rope_base = 10000.0
MESH = pl.DeviceIdType.MESH
F32, BF16 = jnp.float32, jnp.bfloat16


def dot(a, b):
    return jnp.dot(a, b, preferred_element_type=F32)


def dot_tn(a, b):
    return lax.dot_general(a, b, (((0,), (0,)), ((), ())), preferred_element_type=F32)


def dot_nt(a, b):
    return lax.dot_general(a, b, (((1,), (1,)), ((), ())), preferred_element_type=F32)


def remote(src, dst, send, recv, where):
    return pltpu.make_async_remote_copy(
        src_ref=src, dst_ref=dst, send_sem=send, recv_sem=recv, device_id=where, device_id_type=MESH
    )


def rows_of(start, size):
    return pl.ds(pl.multiple_of(start, size), size)


def kernel(
    S,
    T,
    latent,
    cond,
    context,
    norm_gain,
    mod_shift,
    mod_scale,
    mod_gate,
    w_query,
    w_key,
    w_value,
    w_gate,
    w_out,
    decay,
    gain,
    out,
    x_all,
    c_all,
    h_ref,
    hc_ref,
    m_shift,
    m_scale,
    m_gate,
    vq,
    vk,
    vv,
    vg,
    vo,
    m_send,
    m_sp,
    m_tp,
    mod,
    cos_t,
    sin_t,
    q_ref,
    k_ref,
    v_ref,
    ck_ref,
    cv_ref,
    g_ref,
    ret_ref,
    gated,
    loc,
    st_in,
    st_out,
    part,
    p1,
    p2,
    xs,
    xr,
    load_sem,
    lat_send,
    lat_recv,
    ctx_send,
    ctx_fsend,
    ctx_recv,
    msp_send,
    msp_recv,
    mtp_send,
    mtp_recv,
    st_send,
    st_recv,
    p1_send,
    p1_recv,
    p2_send,
    p2_recv,
    x_send,
    x_recv,
):
    sp, tp = lax.axis_index("sp"), lax.axis_index("tp")
    R, D = latent.shape
    Cr = context.shape[0]
    half = Cr // 2
    CT = Cr * S
    span = R * T
    nh = w_query.shape[1] // DK
    DV = w_value.shape[1] // nh
    Mc = mod_shift.shape[1]
    X = T // 2
    chip, core = tp // 2, lax.rem(tp, 2)
    partner = tp + 1 - 2 * core
    is_end = jnp.logical_or(sp == 0, sp == S - 1)
    NC = part.shape[0]
    W = D // NC

    loads = [
        pltpu.make_async_copy(src, dst, load_sem.at[i])
        for i, (src, dst) in enumerate(
            [
                (mod_shift, m_shift),
                (mod_scale, m_scale),
                (mod_gate, m_gate),
                (latent, x_all.at[rows_of(tp * R, R)]),
                (context, c_all.at[rows_of(sp * Cr, Cr)]),
                (w_key, vk),
                (w_value, vv),
                (w_query, vq),
                (w_gate, vg),
                (w_out, vo),
            ]
        )
    ]
    for copy in loads:
        copy.start()

    barrier = pltpu.get_barrier_semaphore()
    for k in range(1, S):
        pl.semaphore_signal(
            barrier, inc=1, device_id={"sp": lax.rem(sp + k, S)}, device_id_type=MESH
        )
    for k in range(1, T):
        pl.semaphore_signal(
            barrier, inc=1, device_id={"tp": lax.rem(tp + k, T)}, device_id_type=MESH
        )
    pl.semaphore_wait(barrier, S + T - 2)

    def lat_copy(src, owner, to, which):
        place = rows_of(owner * R, R)
        return remote(
            latent if src is None else x_all.at[place],
            x_all.at[place],
            lat_send.at[which, to if which == 0 else owner],
            lat_recv.at[owner],
            {"tp": to},
        )

    others = [lax.rem(chip + k, X) for k in range(1, X)]
    direct = [lat_copy(None, tp, 2 * o + core, 0) for o in others] + [
        lat_copy(None, tp, partner, 0)
    ]
    for copy in direct:
        copy.start()

    def ctx_copy(src_ref, owner, part_core, send, recv, where):
        place = rows_of(owner * Cr + part_core * half, half)
        src = context.at[rows_of(part_core * half, half)] if src_ref is None else c_all.at[place]
        return remote(src, c_all.at[place], send, recv, where)

    ends = (0, S - 1)

    def ctx_out(e):
        return ctx_copy(None, sp, core, ctx_send.at[e], ctx_recv.at[0, sp], {"sp": ends[e]})

    for e in range(2):

        @pl.when(sp != ends[e])
        def _():
            ctx_out(e).start()

    for copy in loads[:3]:
        copy.wait()
    rows = cond[...]
    m_send[...] = jnp.zeros_like(m_send)
    m_send[0:2] = dot(rows, m_shift[...])[0:2]
    m_send[2:4] = dot(rows, m_scale[...])[0:2]
    m_send[4:5] = dot(rows, m_gate[...])[0:1]

    def sp_copy(owner, to):
        return remote(m_send, m_sp.at[owner], msp_send.at[to], msp_recv.at[owner], {"sp": to})

    sp_peers = [lax.rem(sp + k, S) for k in range(1, S)]
    tp_peers = [lax.rem(tp + k, T) for k in range(1, T)]
    for p in sp_peers:
        sp_copy(sp, p).start()

    F = DK // 4
    pos = (lax.broadcasted_iota(jnp.int32, (span, 2 * F), 0) + sp * span).astype(F32)
    lane = lax.broadcasted_iota(jnp.int32, (span, 2 * F), 1)
    grid_row = jnp.floor(pos * (1.0 / GRID_W))
    grid_col = pos - grid_row * GRID_W
    freq = jnp.where(lane < F, lane, lane - F).astype(F32)
    angle = jnp.where(lane < F, grid_row, grid_col) * jnp.exp(
        freq * (-math.log(rope_base) / F)
    )
    cos_t[...] = jnp.cos(angle)
    sin_t[...] = jnp.sin(angle)

    total = m_send[...]
    for p in sp_peers:
        sp_copy(p, p).wait_recv()
        total = total + m_sp[p]
    m_tp[tp] = total

    def tp_copy(owner, to):
        return remote(
            m_tp.at[owner], m_tp.at[owner], mtp_send.at[to], mtp_recv.at[owner], {"tp": to}
        )

    for p in tp_peers:
        tp_copy(tp, p).start()

    forwards = []
    for o in others:
        owner = 2 * o + core
        lat_copy(None, owner, owner, 0).wait_recv()
        copy = lat_copy(1, owner, partner, 1)
        copy.start()
        forwards.append(copy)
    loads[3].wait()

    for p in tp_peers:
        tp_copy(p, p).wait_recv()
    for t in range(T):
        mod[:, t * Mc : (t + 1) * Mc] = m_tp[t]

    def modulate(src, dst, start, count, row):
        mult = norm_gain[...].astype(F32) * (1.0 + mod[2 + row : 3 + row, :])
        shift = mod[row : row + 1, :]
        size = min(32, count)

        def lap(i, _):
            place = rows_of(start + i * size, size)
            x = src[place, :].astype(F32)
            scale = lax.rsqrt(jnp.mean(x * x, axis=-1, keepdims=True) + norm_eps)
            dst[place, :] = (x * scale * mult + shift).astype(BF16)
            return 0

        lax.fori_loop(0, count // size, lap, 0)

    modulate(x_all, h_ref, tp * R, R, 0)
    for o in others:
        modulate(x_all, h_ref, (2 * o + core) * R, R, 0)
    lat_copy(None, partner, partner, 0).wait_recv()
    modulate(x_all, h_ref, partner * R, R, 0)
    for o in others:
        owner = 2 * o + 1 - core
        lat_copy(None, owner, owner, 0).wait_recv()
        modulate(x_all, h_ref, owner * R, R, 0)

    scale_k = DK**-0.5

    def rotated(x):
        u, w = x[:, : DK // 2], x[:, DK // 2 :]
        c, s = cos_t[...], sin_t[...]
        return jnp.concatenate([u * c - w * s, w * c + u * s], axis=1).astype(BF16)

    def cols(j, size):
        return pl.ds(pl.multiple_of(j * size, size), size)

    loads[4].wait()

    @pl.when(is_end)
    def _():
        for p in sp_peers:
            ctx_copy(None, p, core, ctx_send.at[0], ctx_recv.at[0, p], {"sp": p}).wait_recv()
            ctx_copy(1, p, core, ctx_fsend.at[p], ctx_recv.at[1, p], {"tp": partner}).start()

    loads[5].wait()

    def key_tile(h, _):
        k_ref[h] = rotated(dot(h_ref[...], vk[:, cols(h, DK)]) * scale_k)
        return 0

    lax.fori_loop(0, nh, key_tile, 0)
    loads[6].wait()

    def value_tile(j, _):
        v_ref[:, cols(j, TILE)] = dot(h_ref[...], vv[:, cols(j, TILE)]).astype(BF16)
        return 0

    lax.fori_loop(0, nh * DV // TILE, value_tile, 0)

    def local_states(h, _):
        k = k_ref[h].astype(F32)
        v = v_ref[:, cols(h, DV)]
        place = lax.broadcasted_iota(jnp.int32, (span, DK), 0).astype(F32)
        fk = (k * jnp.exp(-decay[0, h] * (span - 1.0 - place))).astype(BF16)
        bk = (k * jnp.exp(-decay[1, h] * place)).astype(BF16)
        loc[0, cols(h, DK), :] = dot_tn(fk, v)
        loc[1, cols(h, DK), :] = dot_tn(bk, v)
        return 0

    lax.fori_loop(0, nh, local_states, 0)

    @pl.when(is_end)
    def _():
        for p in sp_peers:
            ctx_copy(
                1, p, 1 - core, ctx_fsend.at[p], ctx_recv.at[1, p], {"tp": partner}
            ).wait_recv()
        modulate(c_all, hc_ref, 0, CT, 1)
        M = min(CT, TILE)
        at_start = sp == 0
        side = jnp.where(at_start, 0, 1)

        def ctx_rows(r, _):
            place = rows_of(r * M, M)

            def ctx_key(h, _):
                ck_ref[h, place, :] = (dot(hc_ref[place, :], vk[:, cols(h, DK)]) * scale_k).astype(
                    BF16
                )
                return 0

            lax.fori_loop(0, nh, ctx_key, 0)

            def ctx_value(j, _):
                cv_ref[place, cols(j, TILE)] = dot(hc_ref[place, :], vv[:, cols(j, TILE)]).astype(
                    BF16
                )
                return 0

            lax.fori_loop(0, nh * DV // TILE, ctx_value, 0)
            return 0

        lax.fori_loop(0, CT // M, ctx_rows, 0)

        def ctx_state(h, _):
            place = lax.broadcasted_iota(jnp.int32, (CT, DK), 0).astype(F32)
            rate = jnp.where(at_start, decay[0, h], decay[1, h])
            away = jnp.where(at_start, CT - 1.0 - place, place)
            keys = (ck_ref[h].astype(F32) * jnp.exp(-rate * away)).astype(BF16)
            state = dot_tn(keys, cv_ref[:, cols(h, DV)]) * gain[h]
            st_in[side, cols(h, DK), :] = state.astype(BF16)
            return 0

        lax.fori_loop(0, nh, ctx_state, 0)

    n = nh * DK // CHUNK
    hop = (sp, S - 1 - sp)
    after = (sp + 1, sp - 1)
    before = (sp - 1, sp + 1)
    per_head = DK // CHUNK

    def st_copy(d, c, to):
        place = rows_of(c * CHUNK, CHUNK)
        return remote(
            st_out.at[d, place],
            st_in.at[d, place],
            st_send.at[d, c],
            st_recv.at[d, c],
            {"sp": to},
        )

    def relay(d, c):
        @pl.when(hop[d] > 0)
        def _():
            st_copy(d, c, before[d]).wait_recv()

        @pl.when(hop[d] < S - 1)
        def _():
            place = rows_of(c * CHUNK, CHUNK)
            fade = jnp.exp(jnp.full((1, DV), -decay[d, c // per_head] * span, F32))
            st_out[d, place, :] = (st_in[d, place, :].astype(F32) * fade + loc[d, place, :]).astype(
                BF16
            )
            st_copy(d, c, after[d]).start()

    ng = nh * DV // TILE
    loads[7].wait()
    loads[8].wait()

    def lap(i, _):
        for d in range(2):
            c = i - LAG * hop[d]

            @pl.when(jnp.logical_and(c >= 0, c < n))
            def _():
                relay(d, c)

        @pl.when(i < nh)
        def _():
            q_ref[i] = rotated(dot(h_ref[...], vq[:, cols(i, DK)]))

        @pl.when(jnp.logical_and(i >= nh, i < nh + ng))
        def _():
            pre = dot(h_ref[...], vg[:, cols(i - nh, TILE)])
            g_ref[:, cols(i - nh, TILE)] = pre / (1.0 + jnp.exp(-pre))

        @pl.when(jnp.logical_and(i >= nh + ng, i < 2 * nh + ng))
        def _():
            h = i - nh - ng
            row = lax.broadcasted_iota(jnp.int32, (span, span), 0)
            col = lax.broadcasted_iota(jnp.int32, (span, span), 1)
            gap = (row - col).astype(F32)
            mask = jnp.where(gap >= 0, jnp.exp(-decay[0, h] * jnp.maximum(gap, 0.0)), 0.0)
            mask += jnp.where(gap <= 0, jnp.exp(-decay[1, h] * jnp.maximum(-gap, 0.0)), 0.0)
            weights = (dot_nt(q_ref[h], k_ref[h]) * mask).astype(BF16)
            ret_ref[h] = dot(weights, v_ref[:, cols(h, DV)])

        return 0

    lax.fori_loop(0, max(n + LAG * (S - 1), 2 * nh + ng), lap, 0)

    def finish(h, _):
        place = lax.broadcasted_iota(jnp.int32, (span, DV), 0).astype(F32)
        q = q_ref[h]
        ret = (
            ret_ref[h]
            + dot(q, st_in[0, cols(h, DK), :]) * jnp.exp(-decay[0, h] * (place + 1.0))
            + dot(q, st_in[1, cols(h, DK), :]) * jnp.exp(-decay[1, h] * (span - place))
        )
        ret = ret - jnp.mean(ret, axis=-1, keepdims=True)
        ret = ret * lax.rsqrt(jnp.mean(ret * ret, axis=-1, keepdims=True) + norm_eps)
        gated[:, cols(h, DV)] = (g_ref[:, cols(h, DV)] * ret).astype(BF16)
        return 0

    lax.fori_loop(0, nh, finish, 0)
    loads[9].wait()

    def p1_copy(c, o):
        return remote(
            part.at[c, 2 * o + 1 - core],
            p1.at[c, o],
            p1_send.at[c, o],
            p1_recv.at[c, o],
            {"tp": partner},
        )

    def p2_copy(c):
        return remote(
            part.at[c, partner], p2.at[c], p2_send.at[c], p2_recv.at[c], {"tp": partner}
        )

    def x_copy(c, owner, o):
        return remote(
            xs.at[c, o], xr.at[c, owner], x_send.at[c, o], x_recv.at[c, owner], {"tp": 2 * o + core}
        )

    def across(c):
        for o in others:
            p1_copy(c, o).wait_recv()
            mine = part[c, 2 * o + core].astype(F32)
            xs[c, o] = (mine + p1[c, o].astype(F32)).astype(BF16)
            x_copy(c, chip, o).start()

    def project(c, _):
        product = dot(gated[...], vo[:, cols(c, W)]).astype(BF16)
        for t in range(T):
            part[c, t] = product[t * R : (t + 1) * R, :]
        for o in others:
            p1_copy(c, o).start()
        p2_copy(c).start()

        @pl.when(c > 0)
        def _():
            across(c - 1)

        return 0

    lax.fori_loop(0, NC, project, 0)
    across(NC - 1)

    def final(c, _):
        p2_copy(c).wait_recv()
        total = part[c, tp].astype(F32) + p2[c].astype(F32)
        for o in others:
            x_copy(c, o, o).wait_recv()
            total = total + xr[c, o].astype(F32)
        mine = x_all[rows_of(tp * R, R), cols(c, W)].astype(F32)
        out[:, cols(c, W)] = (mine + mod[4:5, cols(c, W)] * total).astype(BF16)
        return 0

    lax.fori_loop(0, NC, final, 0)

    for copy in direct + forwards:
        copy.wait_send()
    for e in range(2):

        @pl.when(sp != ends[e])
        def _():
            ctx_out(e).wait_send()

    @pl.when(is_end)
    def _():
        for p in sp_peers:
            ctx_copy(1, p, core, ctx_fsend.at[p], ctx_recv.at[1, p], {"tp": partner}).wait_send()

    for p in sp_peers:
        sp_copy(sp, p).wait_send()
    for p in tp_peers:
        tp_copy(tp, p).wait_send()

    def sent(c, _):
        for d in range(2):

            @pl.when(hop[d] < S - 1)
            def _():
                st_copy(d, c, after[d]).wait_send()

        return 0

    lax.fori_loop(0, n, sent, 0)

    def sent_out(c, _):
        for o in others:
            p1_copy(c, o).wait_send()
            x_copy(c, chip, o).wait_send()
        p2_copy(c).wait_send()
        return 0

    lax.fori_loop(0, NC, sent_out, 0)


def body(
    S,
    T,
    latent,
    cond,
    context,
    context_cond,
    norm_gain,
    mod_shift,
    mod_scale,
    mod_gate,
    w_query,
    w_key,
    w_value,
    w_gate,
    w_out,
    decay_rate,
    context_gain,
):
    R, D = latent.shape
    Cr = context.shape[0]
    span, CT = R * T, Cr * S
    nh = w_query.shape[1] // DK
    DV = w_value.shape[1] // nh
    Mr, Mc = mod_shift.shape
    X = T // 2
    NC = 4
    W = D // NC
    n = nh * DK // CHUNK
    rows = jnp.concatenate(
        [cond[None], context_cond[None], jnp.zeros((14, Mr), cond.dtype)]
    ).astype(F32)
    rows = jax.nn.silu(rows).astype(BF16)
    VMEM = pl.BlockSpec(memory_space=pltpu.VMEM)
    ANY = pl.BlockSpec(memory_space=pl.ANY)
    SMEM = pl.BlockSpec(memory_space=pltpu.SMEM)
    v = pltpu.VMEM
    DMA = pltpu.SemaphoreType.DMA
    return pl.pallas_call(
        functools.partial(kernel, S, T),
        out_shape=jax.ShapeDtypeStruct((R, D), BF16),
        in_specs=[ANY, VMEM, ANY, VMEM] + [ANY] * 8 + [SMEM, SMEM],
        out_specs=VMEM,
        scratch_shapes=[
            v((span, D), BF16),
            v((CT, D), BF16),
            v((span, D), BF16),
            v((CT, D), BF16),
            v((Mr, Mc), BF16),
            v((Mr, Mc), BF16),
            v((Mr, Mc), BF16),
            v(w_query.shape, BF16),
            v(w_key.shape, BF16),
            v(w_value.shape, BF16),
            v(w_gate.shape, BF16),
            v(w_out.shape, BF16),
            v((8, Mc), F32),
            v((S, 8, Mc), F32),
            v((T, 8, Mc), F32),
            v((8, D), F32),
            v((span, DK // 2), F32),
            v((span, DK // 2), F32),
            v((nh, span, DK), BF16),
            v((nh, span, DK), BF16),
            v((span, nh * DV), BF16),
            v((nh, CT, DK), BF16),
            v((CT, nh * DV), BF16),
            v((span, nh * DV), F32),
            v((nh, span, DV), F32),
            v((span, nh * DV), BF16),
            v((2, nh * DK, DV), F32),
            v((2, nh * DK, DV), BF16),
            v((2, nh * DK, DV), BF16),
            v((NC, T, R, W), BF16),
            v((NC, X, R, W), BF16),
            v((NC, R, W), BF16),
            v((NC, X, R, W), BF16),
            v((NC, X, R, W), BF16),
            DMA((10,)),
            DMA((2, T)),
            DMA((T,)),
            DMA((2,)),
            DMA((S,)),
            DMA((2, S)),
            DMA((S,)),
            DMA((S,)),
            DMA((T,)),
            DMA((T,)),
            DMA((2, n)),
            DMA((2, n)),
            DMA((NC, X)),
            DMA((NC, X)),
            DMA((NC,)),
            DMA((NC,)),
            DMA((NC, X)),
            DMA((NC, X)),
        ],
        compiler_params=pltpu.CompilerParams(
            collective_id=0, has_side_effects=True, vmem_limit_bytes=60 * 1024 * 1024
        ),
    )(
        latent,
        rows,
        context,
        norm_gain[None],
        mod_shift,
        mod_scale,
        mod_gate,
        w_query,
        w_key,
        w_value,
        w_gate,
        w_out,
        decay_rate,
        context_gain,
    )


def solution(mesh):
    return jax.shard_map(
        functools.partial(body, mesh.shape["sp"], mesh.shape["tp"]),
        mesh=mesh,
        in_specs=(
            P(("grp", "sp", "tp"), None),
            P(("grp", "sp")),
            P(("grp", "sp"), None),
            P("sp"),
            P(),
            P("sp", "tp"),
            P("sp", "tp"),
            P("sp", "tp"),
            P(None, "tp"),
            P(None, "tp"),
            P(None, "tp"),
            P(None, "tp"),
            P("tp", None),
            P(None, "tp"),
            P("tp"),
        ),
        out_specs=P(("grp", "sp", "tp"), None),
        check_vma=False,
    )
```

```python
import functools
import math

import jax
import jax.numpy as jnp
from jax import lax
from jax.experimental import pallas as pl
from jax.experimental.pallas import tpu as pltpu
from jax.sharding import PartitionSpec as P

DK = 256
GRID_W = 128
TILE = 256
CHUNK = 32
LAG = 2
norm_eps = 1e-06
rope_base = 10000.0
MESH = pl.DeviceIdType.MESH
F32, BF16 = jnp.float32, jnp.bfloat16


def dot(a, b):
    return jnp.dot(a, b, preferred_element_type=F32)


def dot_tn(a, b):
    return lax.dot_general(a, b, (((0,), (0,)), ((), ())), preferred_element_type=F32)


def dot_nt(a, b):
    return lax.dot_general(a, b, (((1,), (1,)), ((), ())), preferred_element_type=F32)


def remote(src, dst, send, recv, where):
    return pltpu.make_async_remote_copy(
        src_ref=src, dst_ref=dst, send_sem=send, recv_sem=recv, device_id=where, device_id_type=MESH
    )


def rows_of(start, size):
    return pl.ds(pl.multiple_of(start, size), size)


def kernel(
    S,
    T,
    latent,
    cond,
    context,
    norm_gain,
    mod_shift,
    mod_scale,
    mod_gate,
    w_query,
    w_key,
    w_value,
    w_gate,
    w_out,
    decay,
    gain,
    out,
    x_all,
    c_all,
    h_ref,
    hc_ref,
    m_shift,
    m_scale,
    m_gate,
    vq,
    vk,
    vv,
    vg,
    vo,
    m_send,
    m_sp,
    m_tp,
    mod,
    cos_t,
    sin_t,
    q_ref,
    k_ref,
    v_ref,
    ck_ref,
    cv_ref,
    g_ref,
    ret_ref,
    gated,
    loc,
    st_in,
    st_out,
    part,
    p1,
    p2,
    xs,
    xr,
    load_sem,
    lat_send,
    lat_recv,
    ctx_send,
    ctx_fsend,
    ctx_recv,
    msp_send,
    msp_recv,
    mtp_send,
    mtp_recv,
    st_send,
    st_recv,
    p1_send,
    p1_recv,
    p2_send,
    p2_recv,
    x_send,
    x_recv,
):
    sp, tp = lax.axis_index("sp"), lax.axis_index("tp")
    R, D = latent.shape
    Cr = context.shape[0]
    half = Cr // 2
    CT = Cr * S
    span = R * T
    nh = w_query.shape[1] // DK
    DV = w_value.shape[1] // nh
    Mc = mod_shift.shape[1]
    X = T // 2
    chip, core = tp // 2, lax.rem(tp, 2)
    partner = tp + 1 - 2 * core
    is_end = jnp.logical_or(sp == 0, sp == S - 1)
    NC = part.shape[0]
    W = D // NC

    loads = [
        pltpu.make_async_copy(src, dst, load_sem.at[i])
        for i, (src, dst) in enumerate(
            [
                (mod_shift, m_shift),
                (mod_scale, m_scale),
                (mod_gate, m_gate),
                (latent, x_all.at[rows_of(tp * R, R)]),
                (context, c_all.at[rows_of(sp * Cr, Cr)]),
                (w_key, vk),
                (w_value, vv),
                (w_query, vq),
                (w_gate, vg),
                (w_out, vo),
            ]
        )
    ]
    for copy in loads:
        copy.start()

    barrier = pltpu.get_barrier_semaphore()
    for k in range(1, S):
        pl.semaphore_signal(
            barrier, inc=1, device_id={"sp": lax.rem(sp + k, S)}, device_id_type=MESH
        )
    for k in range(1, T):
        pl.semaphore_signal(
            barrier, inc=1, device_id={"tp": lax.rem(tp + k, T)}, device_id_type=MESH
        )
    pl.semaphore_wait(barrier, S + T - 2)

    def lat_copy(src, owner, to, which):
        place = rows_of(owner * R, R)
        return remote(
            latent if src is None else x_all.at[place],
            x_all.at[place],
            lat_send.at[which, to if which == 0 else owner],
            lat_recv.at[owner],
            {"tp": to},
        )

    others = [lax.rem(chip + k, X) for k in range(1, X)]
    direct = [lat_copy(None, tp, 2 * o + core, 0) for o in others] + [
        lat_copy(None, tp, partner, 0)
    ]
    for copy in direct:
        copy.start()

    def ctx_copy(src_ref, owner, part_core, send, recv, where):
        place = rows_of(owner * Cr + part_core * half, half)
        src = context.at[rows_of(part_core * half, half)] if src_ref is None else c_all.at[place]
        return remote(src, c_all.at[place], send, recv, where)

    ends = (0, S - 1)

    def ctx_out(e):
        return ctx_copy(None, sp, core, ctx_send.at[e], ctx_recv.at[0, sp], {"sp": ends[e]})

    for e in range(2):

        @pl.when(sp != ends[e])
        def _():
            ctx_out(e).start()

    for copy in loads[:3]:
        copy.wait()
    rows = cond[...]
    m_send[...] = jnp.zeros_like(m_send)
    m_send[0:2] = dot(rows, m_shift[...])[0:2]
    m_send[2:4] = dot(rows, m_scale[...])[0:2]
    m_send[4:5] = dot(rows, m_gate[...])[0:1]

    def sp_copy(owner, to):
        return remote(m_send, m_sp.at[owner], msp_send.at[to], msp_recv.at[owner], {"sp": to})

    sp_peers = [lax.rem(sp + k, S) for k in range(1, S)]
    tp_peers = [lax.rem(tp + k, T) for k in range(1, T)]
    for p in sp_peers:
        sp_copy(sp, p).start()

    F = DK // 4
    pos = (lax.broadcasted_iota(jnp.int32, (span, 2 * F), 0) + sp * span).astype(F32)
    lane = lax.broadcasted_iota(jnp.int32, (span, 2 * F), 1)
    grid_row = jnp.floor(pos * (1.0 / GRID_W))
    grid_col = pos - grid_row * GRID_W
    freq = jnp.where(lane < F, lane, lane - F).astype(F32)
    angle = jnp.where(lane < F, grid_row, grid_col) * jnp.exp(
        freq * (-math.log(rope_base) / F)
    )
    cos_t[...] = jnp.cos(angle)
    sin_t[...] = jnp.sin(angle)

    total = m_send[...]
    for p in sp_peers:
        sp_copy(p, p).wait_recv()
        total = total + m_sp[p]
    m_tp[tp] = total

    def tp_copy(owner, to):
        return remote(
            m_tp.at[owner], m_tp.at[owner], mtp_send.at[to], mtp_recv.at[owner], {"tp": to}
        )

    for p in tp_peers:
        tp_copy(tp, p).start()

    forwards = []
    for o in others:
        owner = 2 * o + core
        lat_copy(None, owner, owner, 0).wait_recv()
        copy = lat_copy(1, owner, partner, 1)
        copy.start()
        forwards.append(copy)
    loads[3].wait()

    for p in tp_peers:
        tp_copy(p, p).wait_recv()
    for t in range(T):
        mod[:, t * Mc : (t + 1) * Mc] = m_tp[t]

    def modulate(src, dst, start, count, row):
        mult = norm_gain[...].astype(F32) * (1.0 + mod[2 + row : 3 + row, :])
        shift = mod[row : row + 1, :]
        size = min(32, count)

        def lap(i, _):
            place = rows_of(start + i * size, size)
            x = src[place, :].astype(F32)
            scale = lax.rsqrt(jnp.mean(x * x, axis=-1, keepdims=True) + norm_eps)
            dst[place, :] = (x * scale * mult + shift).astype(BF16)
            return 0

        lax.fori_loop(0, count // size, lap, 0)

    modulate(x_all, h_ref, tp * R, R, 0)
    for o in others:
        modulate(x_all, h_ref, (2 * o + core) * R, R, 0)
    lat_copy(None, partner, partner, 0).wait_recv()
    modulate(x_all, h_ref, partner * R, R, 0)
    for o in others:
        owner = 2 * o + 1 - core
        lat_copy(None, owner, owner, 0).wait_recv()
        modulate(x_all, h_ref, owner * R, R, 0)

    scale_k = DK**-0.5

    def rotated(x):
        u, w = x[:, : DK // 2], x[:, DK // 2 :]
        c, s = cos_t[...], sin_t[...]
        return jnp.concatenate([u * c - w * s, w * c + u * s], axis=1).astype(BF16)

    def cols(j, size):
        return pl.ds(pl.multiple_of(j * size, size), size)

    loads[4].wait()

    @pl.when(is_end)
    def _():
        for p in sp_peers:
            ctx_copy(None, p, core, ctx_send.at[0], ctx_recv.at[0, p], {"sp": p}).wait_recv()
            ctx_copy(1, p, core, ctx_fsend.at[p], ctx_recv.at[1, p], {"tp": partner}).start()

    loads[5].wait()
    loads[6].wait()
    M = min(CT, TILE)
    tiles = DV // TILE
    at_start = sp == 0
    side = jnp.where(at_start, 0, 1)

    def latent_head(h):
        key = rotated(dot(h_ref[...], vk[:, cols(h, DK)]) * scale_k)
        k_ref[h] = key

        def value_tile(j, _):
            v_ref[:, cols(j, TILE)] = dot(h_ref[...], vv[:, cols(j, TILE)]).astype(BF16)
            return 0

        lax.fori_loop(h * tiles, (h + 1) * tiles, value_tile, 0)
        k = k_ref[h].astype(F32)
        v = v_ref[:, cols(h, DV)]
        place = lax.broadcasted_iota(jnp.int32, (span, DK), 0).astype(F32)
        fk = (k * jnp.exp(-decay[0, h] * (span - 1.0 - place))).astype(BF16)
        bk = (k * jnp.exp(-decay[1, h] * place)).astype(BF16)
        loc[0, cols(h, DK), :] = dot_tn(fk, v)
        loc[1, cols(h, DK), :] = dot_tn(bk, v)

    def context_head(h):
        def ctx_rows(r, _):
            place = rows_of(r * M, M)
            ck_ref[h, place, :] = (dot(hc_ref[place, :], vk[:, cols(h, DK)]) * scale_k).astype(BF16)

            def ctx_value(j, _):
                cv_ref[place, cols(j, TILE)] = dot(hc_ref[place, :], vv[:, cols(j, TILE)]).astype(
                    BF16
                )
                return 0

            lax.fori_loop(h * tiles, (h + 1) * tiles, ctx_value, 0)
            return 0

        lax.fori_loop(0, CT // M, ctx_rows, 0)
        place = lax.broadcasted_iota(jnp.int32, (CT, DK), 0).astype(F32)
        rate = jnp.where(at_start, decay[0, h], decay[1, h])
        away = jnp.where(at_start, CT - 1.0 - place, place)
        keys = (ck_ref[h].astype(F32) * jnp.exp(-rate * away)).astype(BF16)
        state = dot_tn(keys, cv_ref[:, cols(h, DV)]) * gain[h]
        st_in[side, cols(h, DK), :] = state.astype(BF16)

    latent_head(0)

    @pl.when(is_end)
    def _():
        for p in sp_peers:
            ctx_copy(
                1, p, 1 - core, ctx_fsend.at[p], ctx_recv.at[1, p], {"tp": partner}
            ).wait_recv()
        modulate(c_all, hc_ref, 0, CT, 1)
        context_head(0)

    n = nh * DK // CHUNK
    hop = (sp, S - 1 - sp)
    after = (sp + 1, sp - 1)
    before = (sp - 1, sp + 1)
    per_head = DK // CHUNK

    def st_copy(d, c, to):
        place = rows_of(c * CHUNK, CHUNK)
        return remote(
            st_out.at[d, place],
            st_in.at[d, place],
            st_send.at[d, c],
            st_recv.at[d, c],
            {"sp": to},
        )

    def relay(d, c):
        @pl.when(hop[d] > 0)
        def _():
            st_copy(d, c, before[d]).wait_recv()

        @pl.when(hop[d] < S - 1)
        def _():
            place = rows_of(c * CHUNK, CHUNK)
            fade = jnp.exp(jnp.full((1, DV), -decay[d, c // per_head] * span, F32))
            st_out[d, place, :] = (st_in[d, place, :].astype(F32) * fade + loc[d, place, :]).astype(
                BF16
            )
            st_copy(d, c, after[d]).start()

    ng = nh * DV // TILE
    loads[7].wait()
    loads[8].wait()

    inner = max(nh + ng, per_head * (nh - 1) + 1)

    def lap(i, _):
        for h in range(1, nh):

            @pl.when(i == h * per_head)
            def _():
                latent_head(h)

                @pl.when(is_end)
                def _():
                    context_head(h)

        for d in range(2):
            c = i - LAG * hop[d]

            @pl.when(jnp.logical_and(c >= 0, c < n))
            def _():
                relay(d, c)

        @pl.when(i < nh)
        def _():
            q_ref[i] = rotated(dot(h_ref[...], vq[:, cols(i, DK)]))

        @pl.when(jnp.logical_and(i >= nh, i < nh + ng))
        def _():
            pre = dot(h_ref[...], vg[:, cols(i - nh, TILE)])
            g_ref[:, cols(i - nh, TILE)] = pre / (1.0 + jnp.exp(-pre))

        @pl.when(jnp.logical_and(i >= inner, i < inner + nh))
        def _():
            h = i - inner
            row = lax.broadcasted_iota(jnp.int32, (span, span), 0)
            col = lax.broadcasted_iota(jnp.int32, (span, span), 1)
            gap = (row - col).astype(F32)
            mask = jnp.where(gap >= 0, jnp.exp(-decay[0, h] * jnp.maximum(gap, 0.0)), 0.0)
            mask += jnp.where(gap <= 0, jnp.exp(-decay[1, h] * jnp.maximum(-gap, 0.0)), 0.0)
            weights = (dot_nt(q_ref[h], k_ref[h]) * mask).astype(BF16)
            ret_ref[h] = dot(weights, v_ref[:, cols(h, DV)])

        return 0

    lax.fori_loop(0, max(n + LAG * (S - 1), inner + nh), lap, 0)

    def finish(h, _):
        place = lax.broadcasted_iota(jnp.int32, (span, DV), 0).astype(F32)
        q = q_ref[h]
        ret = (
            ret_ref[h]
            + dot(q, st_in[0, cols(h, DK), :]) * jnp.exp(-decay[0, h] * (place + 1.0))
            + dot(q, st_in[1, cols(h, DK), :]) * jnp.exp(-decay[1, h] * (span - place))
        )
        ret = ret - jnp.mean(ret, axis=-1, keepdims=True)
        ret = ret * lax.rsqrt(jnp.mean(ret * ret, axis=-1, keepdims=True) + norm_eps)
        gated[:, cols(h, DV)] = (g_ref[:, cols(h, DV)] * ret).astype(BF16)
        return 0

    lax.fori_loop(0, nh, finish, 0)
    loads[9].wait()

    def p1_copy(c, o):
        return remote(
            part.at[c, 2 * o + 1 - core],
            p1.at[c, o],
            p1_send.at[c, o],
            p1_recv.at[c, o],
            {"tp": partner},
        )

    def p2_copy(c):
        return remote(
            part.at[c, partner], p2.at[c], p2_send.at[c], p2_recv.at[c], {"tp": partner}
        )

    def x_copy(c, owner, o):
        return remote(
            xs.at[c, o], xr.at[c, owner], x_send.at[c, o], x_recv.at[c, owner], {"tp": 2 * o + core}
        )

    def across(c):
        for o in others:
            p1_copy(c, o).wait_recv()
            mine = part[c, 2 * o + core].astype(F32)
            xs[c, o] = (mine + p1[c, o].astype(F32)).astype(BF16)
            x_copy(c, chip, o).start()

    def project(c, _):
        product = dot(gated[...], vo[:, cols(c, W)]).astype(BF16)
        for t in range(T):
            part[c, t] = product[t * R : (t + 1) * R, :]
        for o in others:
            p1_copy(c, o).start()
        p2_copy(c).start()

        @pl.when(c > 0)
        def _():
            across(c - 1)

        return 0

    lax.fori_loop(0, NC, project, 0)
    across(NC - 1)

    def final(c, _):
        p2_copy(c).wait_recv()
        total = part[c, tp].astype(F32) + p2[c].astype(F32)
        for o in others:
            x_copy(c, o, o).wait_recv()
            total = total + xr[c, o].astype(F32)
        mine = x_all[rows_of(tp * R, R), cols(c, W)].astype(F32)
        out[:, cols(c, W)] = (mine + mod[4:5, cols(c, W)] * total).astype(BF16)
        return 0

    lax.fori_loop(0, NC, final, 0)

    for copy in direct + forwards:
        copy.wait_send()
    for e in range(2):

        @pl.when(sp != ends[e])
        def _():
            ctx_out(e).wait_send()

    @pl.when(is_end)
    def _():
        for p in sp_peers:
            ctx_copy(1, p, core, ctx_fsend.at[p], ctx_recv.at[1, p], {"tp": partner}).wait_send()

    for p in sp_peers:
        sp_copy(sp, p).wait_send()
    for p in tp_peers:
        tp_copy(tp, p).wait_send()

    def sent(c, _):
        for d in range(2):

            @pl.when(hop[d] < S - 1)
            def _():
                st_copy(d, c, after[d]).wait_send()

        return 0

    lax.fori_loop(0, n, sent, 0)

    def sent_out(c, _):
        for o in others:
            p1_copy(c, o).wait_send()
            x_copy(c, chip, o).wait_send()
        p2_copy(c).wait_send()
        return 0

    lax.fori_loop(0, NC, sent_out, 0)


def body(
    S,
    T,
    latent,
    cond,
    context,
    context_cond,
    norm_gain,
    mod_shift,
    mod_scale,
    mod_gate,
    w_query,
    w_key,
    w_value,
    w_gate,
    w_out,
    decay_rate,
    context_gain,
):
    R, D = latent.shape
    Cr = context.shape[0]
    span, CT = R * T, Cr * S
    nh = w_query.shape[1] // DK
    DV = w_value.shape[1] // nh
    Mr, Mc = mod_shift.shape
    X = T // 2
    NC = 4
    W = D // NC
    n = nh * DK // CHUNK
    rows = jnp.concatenate(
        [cond[None], context_cond[None], jnp.zeros((14, Mr), cond.dtype)]
    ).astype(F32)
    rows = jax.nn.silu(rows).astype(BF16)
    VMEM = pl.BlockSpec(memory_space=pltpu.VMEM)
    ANY = pl.BlockSpec(memory_space=pl.ANY)
    SMEM = pl.BlockSpec(memory_space=pltpu.SMEM)
    v = pltpu.VMEM
    DMA = pltpu.SemaphoreType.DMA
    return pl.pallas_call(
        functools.partial(kernel, S, T),
        out_shape=jax.ShapeDtypeStruct((R, D), BF16),
        in_specs=[ANY, VMEM, ANY, VMEM] + [ANY] * 8 + [SMEM, SMEM],
        out_specs=VMEM,
        scratch_shapes=[
            v((span, D), BF16),
            v((CT, D), BF16),
            v((span, D), BF16),
            v((CT, D), BF16),
            v((Mr, Mc), BF16),
            v((Mr, Mc), BF16),
            v((Mr, Mc), BF16),
            v(w_query.shape, BF16),
            v(w_key.shape, BF16),
            v(w_value.shape, BF16),
            v(w_gate.shape, BF16),
            v(w_out.shape, BF16),
            v((8, Mc), F32),
            v((S, 8, Mc), F32),
            v((T, 8, Mc), F32),
            v((8, D), F32),
            v((span, DK // 2), F32),
            v((span, DK // 2), F32),
            v((nh, span, DK), BF16),
            v((nh, span, DK), BF16),
            v((span, nh * DV), BF16),
            v((nh, CT, DK), BF16),
            v((CT, nh * DV), BF16),
            v((span, nh * DV), F32),
            v((nh, span, DV), F32),
            v((span, nh * DV), BF16),
            v((2, nh * DK, DV), F32),
            v((2, nh * DK, DV), BF16),
            v((2, nh * DK, DV), BF16),
            v((NC, T, R, W), BF16),
            v((NC, X, R, W), BF16),
            v((NC, R, W), BF16),
            v((NC, X, R, W), BF16),
            v((NC, X, R, W), BF16),
            DMA((10,)),
            DMA((2, T)),
            DMA((T,)),
            DMA((2,)),
            DMA((S,)),
            DMA((2, S)),
            DMA((S,)),
            DMA((S,)),
            DMA((T,)),
            DMA((T,)),
            DMA((2, n)),
            DMA((2, n)),
            DMA((NC, X)),
            DMA((NC, X)),
            DMA((NC,)),
            DMA((NC,)),
            DMA((NC, X)),
            DMA((NC, X)),
        ],
        compiler_params=pltpu.CompilerParams(
            collective_id=0, has_side_effects=True, vmem_limit_bytes=60 * 1024 * 1024
        ),
    )(
        latent,
        rows,
        context,
        norm_gain[None],
        mod_shift,
        mod_scale,
        mod_gate,
        w_query,
        w_key,
        w_value,
        w_gate,
        w_out,
        decay_rate,
        context_gain,
    )


def solution(mesh):
    return jax.shard_map(
        functools.partial(body, mesh.shape["sp"], mesh.shape["tp"]),
        mesh=mesh,
        in_specs=(
            P(("grp", "sp", "tp"), None),
            P(("grp", "sp")),
            P(("grp", "sp"), None),
            P("sp"),
            P(),
            P("sp", "tp"),
            P("sp", "tp"),
            P("sp", "tp"),
            P(None, "tp"),
            P(None, "tp"),
            P(None, "tp"),
            P(None, "tp"),
            P("tp", None),
            P(None, "tp"),
            P("tp"),
        ),
        out_specs=P(("grp", "sp", "tp"), None),
        check_vma=False,
    )
```
